32 devices in a mesh: grp: 2 (over x), ra: 4 (over y, core), cb: 4 (over z).
Axes of the slice: x: 2, y: 2, z: 4, core: 2. Of those that a mesh axis runs over, the one named last changes fastest.
Arguments:
- tokens: bfloat16 [256, 4096], P('grp', 'ra'), parts along dimension 0, may hold values from -400 to 400
- gain_first: float32 [4096], P('ra'), may hold values from 0.1 to 1.9
- up_first: bfloat16 [4096, 16384], P('ra', 'cb'), may hold values from -0.09375 to 0.09375
- down_first: bfloat16 [16384, 4096], P('cb', 'ra'), may hold values from -2 to 2
- gain_second: float32 [4096], P('ra'), may hold values from 0.1 to 1.9
- up_second: bfloat16 [4096, 16384], P('ra', 'cb'), may hold values from -0.09375 to 0.09375
- down_second: bfloat16 [16384, 4096], P('cb', 'ra'), may hold values from -2 to 2
- gain_last: float32 [4096], P('ra'), may hold values from 0.1 to 1.9
Outputs:
- normed_out: bfloat16 [256, 4096], P('grp', 'ra'), parts along dimension 0
The draws below stay inside these ranges and needn't reach their ends.
There are 2 independent parts, one for each index of `grp`. The reference program is written for one: setup_inputs(seed, part) draws one part's arguments, and reference() takes and returns one part's arrays. A program takes and returns all parts, laid end to end along the dimension named above; an argument that names none is the same for every part. Nothing has to cross between parts.
All inputs are finite; a program needn't handle non-finite values.
Results may differ from the reference program's by a relative error of at most 0.0081.
Values may be sent and summed in bfloat16 or wider, within the bound.
A program may use at most 64 MiB of HBM per device.

```python
import math
import jax
import jax.numpy as jnp
from jax import lax

D = 4096
FF = 16384
TOKENS = 128


def draw_tokens(key, part):
    keys = jax.random.split(key, 3)
    row_scales = jnp.exp(jax.random.uniform(keys[1], (TOKENS, 1), jnp.float32) * math.log(10.0))
    rough = 0.6 + 0.8 * jax.random.uniform(keys[2], (1, D), jnp.float32)
    ramp = jnp.exp(jnp.linspace(0.0, math.log(6.0), D).astype(jnp.float32))[None, :]
    base = jnp.clip(jax.random.normal(keys[0], (TOKENS, D), jnp.float32), -4.0, 4.0)
    return (base * row_scales * ramp * rough).astype(jnp.bfloat16)


def group_scales(key, top):
    levels = jax.random.uniform(key, (64,), jnp.float32) * math.log(top)
    scales = jnp.exp(levels)
    scales = scales / jnp.sqrt(jnp.mean(scales * scales))
    return jnp.repeat(scales, D // 64)


def scaled_down(key, top, entries):
    keys = jax.random.split(key, 1)
    columns = group_scales(keys[0], top)
    return jnp.clip(entries * FF ** (-0.5) * columns[None, :], -2.0, 2.0).astype(jnp.bfloat16)


def draw_down_first(key, part):
    inner = jax.random.fold_in(key, 711)
    keys = jax.random.split(inner, 2)
    entries = jnp.clip(jax.random.normal(keys[1], (FF, D), jnp.float32), -5.0, 5.0)
    return scaled_down(keys[0], 10.0, entries)


def draw_down_second(key, part):
    inner = jax.random.fold_in(key, 977)
    keys = jax.random.split(inner, 2)
    entries = jnp.clip(jax.random.normal(keys[1], (FF, D), jnp.float32), -5.0, 5.0)
    return scaled_down(keys[0], 10.0, entries)


def steps_of(key, shape, cuts, least, largest):
    loudness, own = 1.0, jax.random.fold_in(key, 6)
    for axis_at, parts in cuts:
        heights = jnp.exp(jax.random.uniform(jax.random.fold_in(own, axis_at), (parts,), jnp.float32, least / len(cuts), largest / len(cuts)))
        loudness = loudness * jnp.repeat(heights, shape[axis_at] // parts).reshape([-1 if axis == axis_at else 1 for axis in range(len(shape))])
    return loudness


def normal_values(own_key, shape, spread, limit, cuts=(), kind=jnp.bfloat16):
    values = jax.random.normal(own_key, shape, jnp.float32) * spread
    if len(cuts) > 0:
        values = steps_of(own_key, shape, cuts, -0.22, 0.18) * values
    return jnp.clip(values, min=-limit, max=limit).astype(kind)


def setup_inputs(seed: int = 0, part: int = 0) -> dict:
    streams_of = jax.random.split(jax.random.key(seed), 9)
    part_keys = jax.random.split(jax.random.fold_in(streams_of[8], part), 9)
    tokens = draw_tokens(jax.random.fold_in(jax.random.fold_in(streams_of[8], part), 71), part)
    gain_first = jnp.clip(1.0 + 0.18 * jax.random.normal(streams_of[1], (D,), jnp.float32), 0.1, 1.9)
    up_first = normal_values(streams_of[2], (D, FF), D ** -0.5, 0.09375, ((0, 4), (1, 4)))
    down_first = draw_down_first(jax.random.fold_in(streams_of[8], 71), part)
    gain_second = jnp.clip(1.0 + 0.18 * jax.random.normal(streams_of[4], (D,), jnp.float32), 0.1, 1.9)
    up_second = normal_values(streams_of[5], (D, FF), D ** -0.5, 0.09375, ((0, 4), (1, 4)))
    down_second = draw_down_second(jax.random.fold_in(streams_of[8], 71), part)
    gain_last = jnp.clip(1.0 + 0.18 * jax.random.normal(streams_of[7], (D,), jnp.float32), 0.1, 1.9)
    return {"tokens": tokens, "gain_first": gain_first, "up_first": up_first, "down_first": down_first, "gain_second": gain_second, "up_second": up_second, "down_second": down_second, "gain_last": gain_last}


norm_eps = 1e-06
residual_keep = 0.5

def mlp_block(stream, gain, up_weight, down_weight):
    row_scale = lax.rsqrt(lax.optimization_barrier(jnp.mean(stream * stream, axis=1, keepdims=True)) + norm_eps)
    normed = (stream * gain).astype(jnp.bfloat16)
    pre = jnp.dot(normed, up_weight, preferred_element_type=jnp.float32) * row_scale
    activated = jnp.square(jax.nn.relu(pre)).astype(jnp.bfloat16)
    branch_out = jnp.dot(activated, down_weight, preferred_element_type=jnp.float32)
    return residual_keep * stream + branch_out

def reference(tokens, gain_first, up_first, down_first, gain_second, up_second, down_second, gain_last):
    stream = tokens.astype(jnp.float32)
    stream = mlp_block(stream, gain_first, up_first, down_first)
    stream = mlp_block(stream, gain_second, up_second, down_second)
    row_scale = lax.rsqrt(lax.optimization_barrier(jnp.mean(stream * stream, axis=1, keepdims=True)) + norm_eps)
    return (stream * row_scale * gain_last).astype(jnp.bfloat16)
```

```python
import functools

import jax
import jax.numpy as jnp
from jax import lax
from jax.experimental import pallas as pl
from jax.experimental.pallas import tpu as pltpu
from jax.sharding import PartitionSpec as P

norm_eps = 1e-06
residual_keep = 0.5
MESH = pl.DeviceIdType.MESH
LANES = 128
HIDDEN_CHUNK = 256
LAG_PAIR = 2
LAG_CHAIN = 3


def kernel(
    R, C,
    tok, gain_1, gain_2, gain_3, up_1, down_1, up_2, down_2,
    out,
    wu, wd, x, stream, own, s_a, r_a, s_b, r_b, act, r_c, acc, s_i, r_i, s_o, r_o, sq_s, sq_r, scale,
    sem_wu, sem_wd, a_send, a_recv, b_send, b_recv, c_send, c_recv,
    i_send, i_recv, o_send, o_recv, q_send, q_recv,
):
    T, width = tok.shape
    chips = R // 2
    NJ, hc = own.shape[0], own.shape[2]
    NP, dc = s_i.shape[1], s_i.shape[3]
    half = NJ * hc
    ups, downs, gains = (up_1, up_2), (down_1, down_2), (gain_1, gain_2, gain_3)

    r = lax.axis_index("ra")
    c = lax.axis_index("cb")
    core = lax.rem(r, 2)
    y = r // 2
    partner = r + 1 - 2 * core
    on_left = c < C // 2
    depth = jnp.where(on_left, c, C - 1 - c)
    inner = jnp.where(on_left, c + 1, c - 1)
    outer = jnp.where(on_left, lax.max(c - 1, 0), lax.min(c + 1, C - 1))
    middle = C // 2 - 1
    lag = lax.min(NP, LAG_CHAIN * (2 * (middle - depth) + 1))

    def load_up(l, side, j):
        at = (core if side == 1 else 1 - core) * half + j * hc
        return pltpu.make_async_copy(
            ups[l].at[:, pl.ds(pl.multiple_of(at, hc), hc)], wu.at[l, side, j], sem_wu.at[l, side, j]
        )

    def load_down(l, side, j):
        at = (core if side == 1 else 1 - core) * half + j * hc
        return pltpu.make_async_copy(
            downs[l].at[pl.ds(pl.multiple_of(at, hc), hc), :], wd.at[l, side, j], sem_wd.at[l, side, j]
        )

    def remote(src, dst, send, recv, axis, to):
        return pltpu.make_async_remote_copy(
            src_ref=src, dst_ref=dst, send_sem=send, recv_sem=recv, device_id={axis: to}, device_id_type=MESH
        )

    def copy_a(l, j):
        return remote(s_a.at[l, j], r_a.at[l, j], a_send.at[l, j], a_recv.at[l, j], "ra", partner)

    def copy_b(l, k, j):
        to = 2 * lax.rem(y + k, chips) + core
        return remote(s_b.at[l, j], r_b.at[l, k - 1, j], b_send.at[l, k - 1, j], b_recv.at[l, k - 1, j], "ra", to)

    def copy_c(l, j):
        return remote(act.at[l, j], r_c.at[l, j], c_send.at[l, j], c_recv.at[l, j], "ra", partner)

    def copy_i(l, p):
        return remote(s_i.at[l, p], r_i.at[l, p], i_send.at[l, p], i_recv.at[l, p], "cb", inner)

    def copy_o(l, p):
        return remote(s_o.at[l, p], r_o.at[l, 1, p], o_send.at[l, 1, p], o_recv.at[l, 1, p], "cb", outer)

    def copy_in(l, p):
        return remote(s_i.at[l, p], r_o.at[l, 0, p], o_send.at[l, 0, p], o_recv.at[l, 0, p], "cb", inner)

    def copy_q(i, k):
        return remote(
            sq_s.at[i], sq_r.at[i, k - 1], q_send.at[i, k - 1], q_recv.at[i, k - 1], "ra", lax.rem(r + k, R)
        )

    def start_squares(i):
        s = stream[...]
        total = jnp.sum(s * s, axis=1, keepdims=True)
        sq_s[i] = jnp.broadcast_to(total, (T, LANES)).T[0:8, :]
        for k in range(1, R):
            copy_q(i, k).start()

    def finish_squares(i):
        total = sq_s[i]
        for k in range(1, R):
            copy_q(i, k).wait_recv()
            total = total + sq_r[i, k - 1]
        factor = lax.rsqrt(total / (width * R) + norm_eps)
        scale[...] = jnp.broadcast_to(factor[0:1, :], (LANES, T)).T

    def columns(p):
        return pl.ds(pl.multiple_of(p * dc, dc), dc)

    @pl.loop(0, NJ)
    def _(j):
        load_up(0, 0, j).start()
        load_up(0, 1, j).start()

    barrier = pltpu.get_barrier_semaphore()
    for k in range(1, R):
        pl.semaphore_signal(barrier, inc=1, device_id={"ra": lax.rem(r + k, R)}, device_id_type=MESH)
    pl.semaphore_signal(barrier, inc=1, device_id={"cb": inner}, device_id_type=MESH)

    @pl.when(depth > 0)
    def _():
        pl.semaphore_signal(barrier, inc=1, device_id={"cb": outer}, device_id_type=MESH)

    stream[...] = tok[...].astype(jnp.float32)
    x[...] = (stream[...] * gain_1[...]).astype(jnp.bfloat16)
    pl.semaphore_wait(barrier, R + jnp.where(depth > 0, 1, 0))

    for l in range(2):
        start_squares(l)

        def reduce_pair(j):
            copy_a(l, j).wait_recv()
            both = own[j] + r_a[l, j].astype(jnp.float32)
            own[j] = both
            s_b[l, j] = both.astype(jnp.bfloat16)
            for k in range(1, chips):
                copy_b(l, k, j).start()

        @pl.loop(0, NJ)
        def _(j):
            load_up(l, 0, j).wait()
            s_a[l, j] = jnp.dot(x[...], wu[l, 0, j], preferred_element_type=jnp.float32).astype(jnp.bfloat16)
            copy_a(l, j).start()
            load_up(l, 1, j).wait()
            own[j] = jnp.dot(x[...], wu[l, 1, j], preferred_element_type=jnp.float32)
            load_down(l, 1, j).start()
            load_down(l, 0, j).start()

            @pl.when(j >= LAG_PAIR)
            def _():
                reduce_pair(j - LAG_PAIR)

        @pl.loop(max(NJ - LAG_PAIR, 0), NJ)
        def _(j):
            reduce_pair(j)

        finish_squares(l)
        acc[...] = jnp.zeros_like(acc)

        def add_other(j):
            copy_c(l, j).wait_recv()
            load_down(l, 0, j).wait()
            acc[...] += jnp.dot(r_c[l, j], wd[l, 0, j], preferred_element_type=jnp.float32)

        @pl.loop(0, NJ)
        def _(j):
            total = own[j]
            for k in range(1, chips):
                copy_b(l, k, j).wait_recv()
                total = total + r_b[l, k - 1, j].astype(jnp.float32)
            pre = total * scale[:, 0:1]
            act[l, j] = jnp.square(jnp.maximum(pre, 0.0)).astype(jnp.bfloat16)
            copy_c(l, j).start()
            if l == 0:
                load_up(1, 0, j).start()
                load_up(1, 1, j).start()
            load_down(l, 1, j).wait()
            acc[...] += jnp.dot(act[l, j], wd[l, 1, j], preferred_element_type=jnp.float32)

            @pl.when(j >= 1)
            def _():
                add_other(j - 1)

        add_other(NJ - 1)

        def send_inward(p):
            @pl.when(depth > 0)
            def _():
                copy_in(l, p).wait_recv()
                acc[:, columns(p)] += r_o[l, 0, p].astype(jnp.float32)

            s_i[l, p] = acc[:, columns(p)].astype(jnp.bfloat16)

            @pl.when(depth == middle)
            def _():
                copy_i(l, p).start()

            @pl.when(depth < middle)
            def _():
                copy_in(l, p).start()

        def send_outward(p):
            @pl.when(depth == middle)
            def _():
                copy_i(l, p).wait_recv()
                total = s_i[l, p].astype(jnp.float32) + r_i[l, p].astype(jnp.float32)
                s_o[l, p] = total.astype(jnp.bfloat16)

                if middle > 0:
                    copy_o(l, p).start()

                stream[:, columns(p)] = residual_keep * stream[:, columns(p)] + s_o[l, p].astype(jnp.float32)

            if middle > 0:
                @pl.when(depth < middle)
                def _():
                    copy_o(l, p).wait_recv()

                    @pl.when(depth > 0)
                    def _():
                        s_o[l, p] = r_o[l, 1, p]
                        copy_o(l, p).start()

                    stream[:, columns(p)] = (
                        residual_keep * stream[:, columns(p)] + r_o[l, 1, p].astype(jnp.float32)
                    )

            if l == 0:
                x[:, columns(p)] = (stream[:, columns(p)] * gain_2[:, columns(p)]).astype(jnp.bfloat16)

        @pl.loop(0, 2 * NP)
        def _(step):
            @pl.when(step < NP)
            def _():
                send_inward(step)

            @pl.when(jnp.logical_and(step >= lag, step < lag + NP))
            def _():
                send_outward(step - lag)

    start_squares(2)
    finish_squares(2)
    out[...] = (stream[...] * scale[:, 0:1] * gain_3[...]).astype(out.dtype)

    for l in range(2):
        @pl.loop(0, NJ)
        def _(j):
            copy_a(l, j).wait_send()
            for k in range(1, chips):
                copy_b(l, k, j).wait_send()
            copy_c(l, j).wait_send()

        @pl.loop(0, NP)
        def _(p):
            @pl.when(depth == middle)
            def _():
                copy_i(l, p).wait_send()

            @pl.when(depth < middle)
            def _():
                copy_in(l, p).wait_send()

            @pl.when(depth > 0)
            def _():
                copy_o(l, p).wait_send()

    for i in range(3):
        for k in range(1, R):
            copy_q(i, k).wait_send()


def per_device(R, C, tokens, gain_1, up_1, down_1, gain_2, up_2, down_2, gain_3):
    T, width = tokens.shape
    hidden = up_1.shape[1]
    chips = R // 2
    hc = min(HIDDEN_CHUNK, hidden // 2)
    NJ = hidden // 2 // hc
    dc = LANES
    NP = width // dc
    bf16, f32 = jnp.bfloat16, jnp.float32
    dma = pltpu.SemaphoreType.DMA
    others = max(chips - 1, 1)
    scratch = [
        pltpu.VMEM((2, 2, NJ, width, hc), bf16),
        pltpu.VMEM((2, 2, NJ, hc, width), bf16),
        pltpu.VMEM((T, width), bf16),
        pltpu.VMEM((T, width), f32),
        pltpu.VMEM((NJ, T, hc), f32),
        pltpu.VMEM((2, NJ, T, hc), bf16),
        pltpu.VMEM((2, NJ, T, hc), bf16),
        pltpu.VMEM((2, NJ, T, hc), bf16),
        pltpu.VMEM((2, others, NJ, T, hc), bf16),
        pltpu.VMEM((2, NJ, T, hc), bf16),
        pltpu.VMEM((2, NJ, T, hc), bf16),
        pltpu.VMEM((T, width), f32),
        pltpu.VMEM((2, NP, T, dc), bf16),
        pltpu.VMEM((2, NP, T, dc), bf16),
        pltpu.VMEM((2, NP, T, dc), bf16),
        pltpu.VMEM((2, 2, NP, T, dc), bf16),
        pltpu.VMEM((3, 8, T), f32),
        pltpu.VMEM((3, R - 1, 8, T), f32),
        pltpu.VMEM((T, LANES), f32),
        dma((2, 2, NJ)), dma((2, 2, NJ)),
        dma((2, NJ)), dma((2, NJ)),
        dma((2, others, NJ)), dma((2, others, NJ)),
        dma((2, NJ)), dma((2, NJ)),
        dma((2, NP)), dma((2, NP)),
        dma((2, 2, NP)), dma((2, 2, NP)),
        dma((3, R - 1)), dma((3, R - 1)),
    ]
    vmem, hbm = pl.BlockSpec(memory_space=pltpu.VMEM), pl.BlockSpec(memory_space=pl.ANY)
    return pl.pallas_call(
        functools.partial(kernel, R, C),
        out_shape=jax.ShapeDtypeStruct((T, width), bf16),
        in_specs=[vmem] * 4 + [hbm] * 4,
        out_specs=vmem,
        scratch_shapes=scratch,
        compiler_params=pltpu.CompilerParams(
            collective_id=0, has_side_effects=True, vmem_limit_bytes=60 * 1024 * 1024
        ),
    )(
        tokens, gain_1.reshape(1, width), gain_2.reshape(1, width), gain_3.reshape(1, width),
        up_1, down_1, up_2, down_2,
    )


def solution(mesh):
    in_specs = (
        P("grp", "ra"),
        P("ra"),
        P("ra", "cb"),
        P("cb", "ra"),
        P("ra"),
        P("ra", "cb"),
        P("cb", "ra"),
        P("ra"),
    )
    return jax.shard_map(
        functools.partial(per_device, mesh.shape["ra"], mesh.shape["cb"]),
        mesh=mesh, in_specs=in_specs, out_specs=P("grp", "ra"), check_vma=False,
    )
```

```python
import functools

import jax
import jax.numpy as jnp
from jax import lax
from jax.experimental import pallas as pl
from jax.experimental.pallas import tpu as pltpu
from jax.sharding import PartitionSpec as P

norm_eps = 1e-06
residual_keep = 0.5
MESH = pl.DeviceIdType.MESH
LANES = 128
HIDDEN_CHUNK = 512
LAG_PAIR = 2
SKIP = 2
CHAIN_CHUNK = 256


def kernel(
    R, C,
    tok, gain_1, gain_2, gain_3, up_1, down_1, up_2, down_2,
    out,
    wu, wd, x, stream, own, s_a, r_a, s_b, r_b, act, r_c, acc, s_i, r_i, s_o, r_o, sq_s, sq_r, scale,
    sem_wu, sem_wd, a_send, a_recv, b_send, b_recv, c_send, c_recv,
    i_send, i_recv, o_send, o_recv, q_send, q_recv,
):
    T, width = tok.shape
    chips = R // 2
    NJ, hc = own.shape[1], own.shape[3]
    NP, dc = s_i.shape[1], s_i.shape[3]
    half = NJ * hc
    ups, downs, gains = (up_1, up_2), (down_1, down_2), (gain_1, gain_2, gain_3)

    r = lax.axis_index("ra")
    c = lax.axis_index("cb")
    core = lax.rem(r, 2)
    y = r // 2
    partner = r + 1 - 2 * core
    on_left = c < C // 2
    depth = jnp.where(on_left, c, C - 1 - c)
    inner = jnp.where(on_left, c + 1, c - 1)
    outer = jnp.where(on_left, lax.max(c - 1, 0), lax.min(c + 1, C - 1))
    middle = C // 2 - 1
    half_T = T // 2

    def load_up(l, side, j):
        at = (core if side == 1 else 1 - core) * half + j * hc
        return pltpu.make_async_copy(
            ups[l].at[:, pl.ds(pl.multiple_of(at, hc), hc)], wu.at[l, side, j], sem_wu.at[l, side, j]
        )

    def load_down(l, side, j):
        at = (core if side == 1 else 1 - core) * half + j * hc
        return pltpu.make_async_copy(
            downs[l].at[pl.ds(pl.multiple_of(at, hc), hc), :], wd.at[l, side, j], sem_wd.at[l, side, j]
        )

    def remote(src, dst, send, recv, axis, to):
        return pltpu.make_async_remote_copy(
            src_ref=src, dst_ref=dst, send_sem=send, recv_sem=recv, device_id={axis: to}, device_id_type=MESH
        )

    def rows(h):
        return pl.ds(h * half_T, half_T)

    def copy_a(s, j):
        return remote(s_a.at[s, j], r_a.at[s, j], a_send.at[s, j], a_recv.at[s, j], "ra", partner)

    def copy_b(s, k, j):
        to = 2 * lax.rem(y + k, chips) + core
        return remote(s_b.at[s, j], r_b.at[s, k - 1, j], b_send.at[s, k - 1, j], b_recv.at[s, k - 1, j], "ra", to)

    def copy_c(s, j):
        return remote(act.at[s, j], r_c.at[s, j], c_send.at[s, j], c_recv.at[s, j], "ra", partner)

    def copy_i(s, p):
        return remote(s_i.at[s, p], r_i.at[s, p], i_send.at[s, p], i_recv.at[s, p], "cb", inner)

    def copy_o(s, p):
        return remote(s_o.at[s, p], r_o.at[s, 1, p], o_send.at[s, 1, p], o_recv.at[s, 1, p], "cb", outer)

    def copy_in(s, p):
        return remote(s_i.at[s, p], r_o.at[s, 0, p], o_send.at[s, 0, p], o_recv.at[s, 0, p], "cb", inner)

    def copy_q(i, k):
        return remote(
            sq_s.at[i], sq_r.at[i, k - 1], q_send.at[i, k - 1], q_recv.at[i, k - 1], "ra", lax.rem(r + k, R)
        )

    def start_squares(i, halves):
        parts = []
        for h in halves:
            s = stream[rows(h), :]
            total = jnp.sum(s * s, axis=1, keepdims=True)
            parts.append(jnp.broadcast_to(total, (half_T, LANES)))
        if len(parts) == 1:
            parts = parts * 2
        sq_s[i] = jnp.concatenate(parts, axis=0).T[0:8, :]
        for k in range(1, R):
            copy_q(i, k).start()

    def finish_squares(i, halves):
        total = sq_s[i]
        for k in range(1, R):
            copy_q(i, k).wait_recv()
            total = total + sq_r[i, k - 1]
        factor = lax.rsqrt(total / (width * R) + norm_eps)
        spread = jnp.broadcast_to(factor[0:1, :], (LANES, T)).T
        for h in halves:
            scale[rows(h), :] = spread[h * half_T:(h + 1) * half_T, :]

    def columns(p):
        return pl.ds(pl.multiple_of(p * dc, dc), dc)

    def reduce_pair(s, h, j):
        copy_a(s, j).wait_recv()
        both = own[h, j] + r_a[s, j].astype(jnp.float32)
        own[h, j] = both
        s_b[s, j] = both.astype(jnp.bfloat16)
        for k in range(1, chips):
            copy_b(s, k, j).start()

    def up(l, h, hook=None):
        s = 2 * l + h

        @pl.loop(0, NJ)
        def _(j):
            if h == 0:
                load_up(l, 0, j).wait()
            s_a[s, j] = jnp.dot(
                x[rows(h), :], wu[l, 0, j], preferred_element_type=jnp.float32
            ).astype(jnp.bfloat16)
            copy_a(s, j).start()
            if h == 0:
                load_up(l, 1, j).wait()
            own[h, j] = jnp.dot(x[rows(h), :], wu[l, 1, j], preferred_element_type=jnp.float32)
            if h == 0:
                load_down(l, 1, j).start()
                load_down(l, 0, j).start()

            @pl.when(j >= LAG_PAIR)
            def _():
                reduce_pair(s, h, j - LAG_PAIR)

            if hook is not None:
                hook(j)

        @pl.loop(max(NJ - LAG_PAIR, 0), NJ)
        def _(j):
            reduce_pair(s, h, j)

    def down(l, h, hook=None):
        s = 2 * l + h
        acc[h] = jnp.zeros((half_T, width), jnp.float32)

        def add_other(j):
            copy_c(s, j).wait_recv()
            if h == 0:
                load_down(l, 0, j).wait()
            acc[h] += jnp.dot(r_c[s, j], wd[l, 0, j], preferred_element_type=jnp.float32)

        @pl.loop(0, NJ)
        def _(j):
            total = own[h, j]
            for k in range(1, chips):
                copy_b(s, k, j).wait_recv()
                total = total + r_b[s, k - 1, j].astype(jnp.float32)
            pre = total * scale[rows(h), 0:1]
            act[s, j] = jnp.square(jnp.maximum(pre, 0.0)).astype(jnp.bfloat16)
            copy_c(s, j).start()
            if h == 0:
                if l == 0:
                    load_up(1, 0, j).start()
                    load_up(1, 1, j).start()
                load_down(l, 1, j).wait()
            acc[h] += jnp.dot(act[s, j], wd[l, 1, j], preferred_element_type=jnp.float32)

            @pl.when(j >= 1)
            def _():
                add_other(j - 1)

            if hook is not None:
                hook(j)

        add_other(NJ - 1)

    def send_inward(l, h, p):
        s = 2 * l + h

        @pl.when(depth > 0)
        def _():
            copy_in(s, p).wait_recv()
            acc[h, :, columns(p)] += r_o[s, 0, p].astype(jnp.float32)

        s_i[s, p] = acc[h, :, columns(p)].astype(jnp.bfloat16)

        @pl.when(depth == middle)
        def _():
            copy_i(s, p).start()

        @pl.when(depth < middle)
        def _():
            copy_in(s, p).start()

    def send_outward(l, h, p):
        s = 2 * l + h

        def add(branch):
            stream[rows(h), columns(p)] = residual_keep * stream[rows(h), columns(p)] + branch.astype(jnp.float32)

        @pl.when(depth == middle)
        def _():
            copy_i(s, p).wait_recv()
            total = s_i[s, p].astype(jnp.float32) + r_i[s, p].astype(jnp.float32)
            s_o[s, p] = total.astype(jnp.bfloat16)
            if middle > 0:
                copy_o(s, p).start()
            add(s_o[s, p])

        if middle > 0:
            @pl.when(depth < middle)
            def _():
                copy_o(s, p).wait_recv()

                @pl.when(depth > 0)
                def _():
                    s_o[s, p] = r_o[s, 1, p]
                    copy_o(s, p).start()

                add(r_o[s, 1, p])

        if l == 0:
            x[rows(h), columns(p)] = (stream[rows(h), columns(p)] * gain_2[:, columns(p)]).astype(jnp.bfloat16)

    def inward_if(inside, l, h, first, last):
        @pl.when((depth == middle) if inside else (depth < middle))
        def _():
            @pl.loop(first, last)
            def _(p):
                send_inward(l, h, p)

    def outward(l, h):
        @pl.loop(0, NP)
        def _(p):
            send_outward(l, h, p)

    @pl.loop(0, NJ)
    def _(j):
        load_up(0, 0, j).start()
        load_up(0, 1, j).start()

    barrier = pltpu.get_barrier_semaphore()
    for k in range(1, R):
        pl.semaphore_signal(barrier, inc=1, device_id={"ra": lax.rem(r + k, R)}, device_id_type=MESH)
    pl.semaphore_signal(barrier, inc=1, device_id={"cb": inner}, device_id_type=MESH)

    @pl.when(depth > 0)
    def _():
        pl.semaphore_signal(barrier, inc=1, device_id={"cb": outer}, device_id_type=MESH)

    stream[...] = tok[...].astype(jnp.float32)
    x[...] = (stream[...] * gain_1[...]).astype(jnp.bfloat16)
    pl.semaphore_wait(barrier, R + jnp.where(depth > 0, 1, 0))

    start_squares(0, (0, 1))
    up(0, 0)
    up(0, 1)
    finish_squares(0, (0, 1))

    for l in range(2):
        if l == 1:
            finish_squares(1, (0,))
        down(l, 0)
        inward_if(False, l, 0, 0, NP)
        if l == 1:
            finish_squares(2, (1,))

        def in_down(j):
            @pl.when(jnp.logical_and(depth == middle, jnp.logical_and(j >= SKIP, j < NP + SKIP)))
            def _():
                send_inward(l, 0, j - SKIP)

        down(l, 1, in_down)
        inward_if(False, l, 1, 0, NP)
        inward_if(True, l, 0, min(NP, max(NJ - SKIP, 0)), NP)
        outward(l, 0)
        if l == 0:
            start_squares(1, (0,))

            def in_up(j):
                @pl.when(jnp.logical_and(depth == middle, j < NP))
                def _():
                    send_inward(0, 1, j)

            up(1, 0, in_up)
            inward_if(True, l, 1, min(NJ, NP), NP)
            outward(l, 1)
            start_squares(2, (1,))
            up(1, 1)
        else:
            start_squares(3, (0,))
            inward_if(True, l, 1, 0, NP)
            outward(l, 1)
            start_squares(4, (1,))

    finish_squares(3, (0,))
    finish_squares(4, (1,))
    out[...] = (stream[...] * scale[:, 0:1] * gain_3[...]).astype(out.dtype)

    for s in range(4):
        @pl.loop(0, NJ)
        def _(j):
            copy_a(s, j).wait_send()
            for k in range(1, chips):
                copy_b(s, k, j).wait_send()
            copy_c(s, j).wait_send()

        @pl.loop(0, NP)
        def _(p):
            @pl.when(depth == middle)
            def _():
                copy_i(s, p).wait_send()

            @pl.when(depth < middle)
            def _():
                copy_in(s, p).wait_send()

            @pl.when(depth > 0)
            def _():
                copy_o(s, p).wait_send()

    for i in range(5):
        for k in range(1, R):
            copy_q(i, k).wait_send()


def per_device(R, C, tokens, gain_1, up_1, down_1, gain_2, up_2, down_2, gain_3):
    T, width = tokens.shape
    hidden = up_1.shape[1]
    chips = R // 2
    hc = min(HIDDEN_CHUNK, hidden // 2)
    NJ = hidden // 2 // hc
    half_T = T // 2
    dc = min(CHAIN_CHUNK, width)
    NP = width // dc
    bf16, f32 = jnp.bfloat16, jnp.float32
    dma = pltpu.SemaphoreType.DMA
    others = max(chips - 1, 1)
    scratch = [
        pltpu.VMEM((2, 2, NJ, width, hc), bf16),
        pltpu.VMEM((2, 2, NJ, hc, width), bf16),
        pltpu.VMEM((T, width), bf16),
        pltpu.VMEM((T, width), f32),
        pltpu.VMEM((2, NJ, half_T, hc), f32),
        pltpu.VMEM((4, NJ, half_T, hc), bf16),
        pltpu.VMEM((4, NJ, half_T, hc), bf16),
        pltpu.VMEM((4, NJ, half_T, hc), bf16),
        pltpu.VMEM((4, others, NJ, half_T, hc), bf16),
        pltpu.VMEM((4, NJ, half_T, hc), bf16),
        pltpu.VMEM((4, NJ, half_T, hc), bf16),
        pltpu.VMEM((2, half_T, width), f32),
        pltpu.VMEM((4, NP, half_T, dc), bf16),
        pltpu.VMEM((4, NP, half_T, dc), bf16),
        pltpu.VMEM((4, NP, half_T, dc), bf16),
        pltpu.VMEM((4, 2, NP, half_T, dc), bf16),
        pltpu.VMEM((5, 8, T), f32),
        pltpu.VMEM((5, R - 1, 8, T), f32),
        pltpu.VMEM((T, LANES), f32),
        dma((2, 2, NJ)), dma((2, 2, NJ)),
        dma((4, NJ)), dma((4, NJ)),
        dma((4, others, NJ)), dma((4, others, NJ)),
        dma((4, NJ)), dma((4, NJ)),
        dma((4, NP)), dma((4, NP)),
        dma((4, 2, NP)), dma((4, 2, NP)),
        dma((5, R - 1)), dma((5, R - 1)),
    ]
    vmem, hbm = pl.BlockSpec(memory_space=pltpu.VMEM), pl.BlockSpec(memory_space=pl.ANY)
    return pl.pallas_call(
        functools.partial(kernel, R, C),
        out_shape=jax.ShapeDtypeStruct((T, width), bf16),
        in_specs=[vmem] * 4 + [hbm] * 4,
        out_specs=vmem,
        scratch_shapes=scratch,
        compiler_params=pltpu.CompilerParams(
            collective_id=0, has_side_effects=True, vmem_limit_bytes=60 * 1024 * 1024
        ),
    )(
        tokens, gain_1.reshape(1, width), gain_2.reshape(1, width), gain_3.reshape(1, width),
        up_1, down_1, up_2, down_2,
    )


def solution(mesh):
    in_specs = (
        P("grp", "ra"),
        P("ra"),
        P("ra", "cb"),
        P("cb", "ra"),
        P("ra"),
        P("ra", "cb"),
        P("cb", "ra"),
        P("ra"),
    )
    return jax.shard_map(
        functools.partial(per_device, mesh.shape["ra"], mesh.shape["cb"]),
        mesh=mesh, in_specs=in_specs, out_specs=P("grp", "ra"), check_vma=False,
    )
```

```python
import functools

import jax
import jax.numpy as jnp
from jax import lax
from jax.experimental import pallas as pl
from jax.experimental.pallas import tpu as pltpu
from jax.sharding import PartitionSpec as P

norm_eps = 1e-06
residual_keep = 0.5
MESH = pl.DeviceIdType.MESH
LANES = 128
HIDDEN_CHUNK = 512
LAG_PAIR = 1
SKIP = 2
CHAIN_CHUNK = 512


def kernel(
    R, C,
    tok, gain_1, gain_2, gain_3, up_1, down_1, up_2, down_2,
    out,
    wu, wd, x, stream, own, s_a, r_a, s_b, r_b, act, r_c, acc, s_i, r_i, s_o, r_o, sq_s, sq_r, scale,
    sem_wu, sem_wd, a_send, a_recv, b_send, b_recv, c_send, c_recv,
    i_send, i_recv, o_send, o_recv, q_send, q_recv,
):
    T, width = tok.shape
    chips = R // 2
    NJ, hc = own.shape[1], own.shape[3]
    NP, dc = s_i.shape[1], s_i.shape[3]
    half = NJ * hc
    ups, downs, gains = (up_1, up_2), (down_1, down_2), (gain_1, gain_2, gain_3)

    r = lax.axis_index("ra")
    c = lax.axis_index("cb")
    core = lax.rem(r, 2)
    y = r // 2
    partner = r + 1 - 2 * core
    on_left = c < C // 2
    depth = jnp.where(on_left, c, C - 1 - c)
    inner = jnp.where(on_left, c + 1, c - 1)
    outer = jnp.where(on_left, lax.max(c - 1, 0), lax.min(c + 1, C - 1))
    middle = C // 2 - 1
    half_T = T // 2

    def load_up(l, side, j):
        at = (core if side == 1 else 1 - core) * half + j * hc
        return pltpu.make_async_copy(
            ups[l].at[:, pl.ds(pl.multiple_of(at, hc), hc)], wu.at[l, j, :, pl.ds(side * hc, hc)], sem_wu.at[l, side, j]
        )

    def load_down(l, side, j):
        at = (core if side == 1 else 1 - core) * half + j * hc
        return pltpu.make_async_copy(
            downs[l].at[pl.ds(pl.multiple_of(at, hc), hc), :], wd.at[l, side, j], sem_wd.at[l, side, j]
        )

    def remote(src, dst, send, recv, axis, to):
        return pltpu.make_async_remote_copy(
            src_ref=src, dst_ref=dst, send_sem=send, recv_sem=recv, device_id={axis: to}, device_id_type=MESH
        )

    def rows(h):
        return pl.ds(h * half_T, half_T)

    def copy_a(s, j):
        return remote(s_a.at[s, j], r_a.at[s, j], a_send.at[s, j], a_recv.at[s, j], "ra", partner)

    def copy_b(s, k, j):
        to = 2 * lax.rem(y + k, chips) + core
        return remote(s_b.at[s, j], r_b.at[s, k - 1, j], b_send.at[s, k - 1, j], b_recv.at[s, k - 1, j], "ra", to)

    def copy_c(s, j):
        return remote(act.at[s, j], r_c.at[s, j], c_send.at[s, j], c_recv.at[s, j], "ra", partner)

    def copy_i(s, p):
        return remote(s_i.at[s, p], r_i.at[s, p], i_send.at[s, p], i_recv.at[s, p], "cb", inner)

    def copy_o(s, p):
        return remote(s_o.at[s, p], r_o.at[s, 1, p], o_send.at[s, 1, p], o_recv.at[s, 1, p], "cb", outer)

    def copy_in(s, p):
        return remote(s_i.at[s, p], r_o.at[s, 0, p], o_send.at[s, 0, p], o_recv.at[s, 0, p], "cb", inner)

    def copy_q(i, k):
        return remote(
            sq_s.at[i], sq_r.at[i, k - 1], q_send.at[i, k - 1], q_recv.at[i, k - 1], "ra", lax.rem(r + k, R)
        )

    def start_squares(i, halves):
        parts = []
        for h in halves:
            s = stream[rows(h), :]
            total = jnp.sum(s * s, axis=1, keepdims=True)
            parts.append(jnp.broadcast_to(total, (half_T, LANES)))
        if len(parts) == 1:
            parts = parts * 2
        sq_s[i] = jnp.concatenate(parts, axis=0).T[0:8, :]
        for k in range(1, R):
            copy_q(i, k).start()

    def finish_squares(i, halves):
        total = sq_s[i]
        for k in range(1, R):
            copy_q(i, k).wait_recv()
            total = total + sq_r[i, k - 1]
        factor = lax.rsqrt(total / (width * R) + norm_eps)
        spread = jnp.broadcast_to(factor[0:1, :], (LANES, T)).T
        for h in halves:
            scale[rows(h), :] = spread[h * half_T:(h + 1) * half_T, :]

    def columns(p):
        return pl.ds(pl.multiple_of(p * dc, dc), dc)

    def reduce_pair(s, h, j):
        copy_a(s, j).wait_recv()
        both = own[h, j] + r_a[s, j].astype(jnp.float32)
        own[h, j] = both
        s_b[s, j] = both.astype(jnp.bfloat16)
        for k in range(1, chips):
            copy_b(s, k, j).start()

    def up(l, h, hook=None):
        s = 2 * l + h

        @pl.loop(0, NJ)
        def _(j):
            if h == 0:
                load_up(l, 0, j).wait()
                load_up(l, 1, j).wait()
            sides = jnp.dot(x[rows(h), :], wu[l, j], preferred_element_type=jnp.float32)
            s_a[s, j] = sides[:, :hc].astype(jnp.bfloat16)
            copy_a(s, j).start()
            own[h, j] = sides[:, hc:]
            if h == 0:
                load_down(l, 1, j).start()
                load_down(l, 0, j).start()

            @pl.when(j >= LAG_PAIR)
            def _():
                reduce_pair(s, h, j - LAG_PAIR)

            if hook is not None:
                hook(j)

        @pl.loop(max(NJ - LAG_PAIR, 0), NJ)
        def _(j):
            reduce_pair(s, h, j)

    def down(l, h, hook=None):
        s = 2 * l + h
        acc[h] = jnp.zeros((half_T, width), jnp.float32)

        def add_other(j):
            copy_c(s, j).wait_recv()
            if h == 0:
                load_down(l, 0, j).wait()
            acc[h] += jnp.dot(r_c[s, j], wd[l, 0, j], preferred_element_type=jnp.float32)

        @pl.loop(0, NJ)
        def _(j):
            total = own[h, j]
            for k in range(1, chips):
                copy_b(s, k, j).wait_recv()
                total = total + r_b[s, k - 1, j].astype(jnp.float32)
            pre = total * scale[rows(h), 0:1]
            act[s, j] = jnp.square(jnp.maximum(pre, 0.0)).astype(jnp.bfloat16)
            copy_c(s, j).start()
            if h == 0:
                if l == 0:
                    load_up(1, 0, j).start()
                    load_up(1, 1, j).start()
                load_down(l, 1, j).wait()
            acc[h] += jnp.dot(act[s, j], wd[l, 1, j], preferred_element_type=jnp.float32)

            @pl.when(j >= 1)
            def _():
                add_other(j - 1)

            if hook is not None:
                hook(j)

        add_other(NJ - 1)

    def send_inward(l, h, p):
        s = 2 * l + h

        @pl.when(depth > 0)
        def _():
            copy_in(s, p).wait_recv()
            acc[h, :, columns(p)] += r_o[s, 0, p].astype(jnp.float32)

        s_i[s, p] = acc[h, :, columns(p)].astype(jnp.bfloat16)

        @pl.when(depth == middle)
        def _():
            copy_i(s, p).start()

        @pl.when(depth < middle)
        def _():
            copy_in(s, p).start()

    def send_outward(l, h, p):
        s = 2 * l + h

        def add(branch):
            stream[rows(h), columns(p)] = residual_keep * stream[rows(h), columns(p)] + branch.astype(jnp.float32)

        @pl.when(depth == middle)
        def _():
            copy_i(s, p).wait_recv()
            total = s_i[s, p].astype(jnp.float32) + r_i[s, p].astype(jnp.float32)
            s_o[s, p] = total.astype(jnp.bfloat16)
            if middle > 0:
                copy_o(s, p).start()
            add(s_o[s, p])

        if middle > 0:
            @pl.when(depth < middle)
            def _():
                copy_o(s, p).wait_recv()

                @pl.when(depth > 0)
                def _():
                    s_o[s, p] = r_o[s, 1, p]
                    copy_o(s, p).start()

                add(r_o[s, 1, p])

        if l == 0:
            x[rows(h), columns(p)] = (stream[rows(h), columns(p)] * gain_2[:, columns(p)]).astype(jnp.bfloat16)

    def inward_if(inside, l, h, first, last):
        @pl.when((depth == middle) if inside else (depth < middle))
        def _():
            @pl.loop(first, last)
            def _(p):
                send_inward(l, h, p)

    def outward(l, h):
        @pl.loop(0, NP)
        def _(p):
            send_outward(l, h, p)

    @pl.loop(0, NJ)
    def _(j):
        load_up(0, 0, j).start()
        load_up(0, 1, j).start()

    barrier = pltpu.get_barrier_semaphore()
    for k in range(1, R):
        pl.semaphore_signal(barrier, inc=1, device_id={"ra": lax.rem(r + k, R)}, device_id_type=MESH)
    pl.semaphore_signal(barrier, inc=1, device_id={"cb": inner}, device_id_type=MESH)

    @pl.when(depth > 0)
    def _():
        pl.semaphore_signal(barrier, inc=1, device_id={"cb": outer}, device_id_type=MESH)

    stream[...] = tok[...].astype(jnp.float32)
    x[...] = (stream[...] * gain_1[...]).astype(jnp.bfloat16)
    pl.semaphore_wait(barrier, R + jnp.where(depth > 0, 1, 0))

    start_squares(0, (0, 1))
    up(0, 0)
    up(0, 1)
    finish_squares(0, (0, 1))

    for l in range(2):
        if l == 1:
            finish_squares(1, (0,))
        down(l, 0)
        inward_if(False, l, 0, 0, NP)
        if l == 1:
            finish_squares(2, (1,))

        def in_down(j):
            @pl.when(jnp.logical_and(depth == middle, jnp.logical_and(j >= SKIP, j < NP + SKIP)))
            def _():
                send_inward(l, 0, j - SKIP)

        down(l, 1, in_down)
        inward_if(False, l, 1, 0, NP)
        inward_if(True, l, 0, min(NP, max(NJ - SKIP, 0)), NP)
        outward(l, 0)
        if l == 0:
            start_squares(1, (0,))

            def in_up(j):
                @pl.when(jnp.logical_and(depth == middle, j < NP))
                def _():
                    send_inward(0, 1, j)

            up(1, 0, in_up)
            inward_if(True, l, 1, min(NJ, NP), NP)
            outward(l, 1)
            start_squares(2, (1,))
            up(1, 1)
        else:
            start_squares(3, (0,))
            inward_if(True, l, 1, 0, NP)
            outward(l, 1)
            start_squares(4, (1,))

    finish_squares(3, (0,))
    finish_squares(4, (1,))
    out[...] = (stream[...] * scale[:, 0:1] * gain_3[...]).astype(out.dtype)

    for s in range(4):
        @pl.loop(0, NJ)
        def _(j):
            copy_a(s, j).wait_send()
            for k in range(1, chips):
                copy_b(s, k, j).wait_send()
            copy_c(s, j).wait_send()

        @pl.loop(0, NP)
        def _(p):
            @pl.when(depth == middle)
            def _():
                copy_i(s, p).wait_send()

            @pl.when(depth < middle)
            def _():
                copy_in(s, p).wait_send()

            @pl.when(depth > 0)
            def _():
                copy_o(s, p).wait_send()

    for i in range(5):
        for k in range(1, R):
            copy_q(i, k).wait_send()


def per_device(R, C, tokens, gain_1, up_1, down_1, gain_2, up_2, down_2, gain_3):
    T, width = tokens.shape
    hidden = up_1.shape[1]
    chips = R // 2
    hc = min(HIDDEN_CHUNK, hidden // 2)
    NJ = hidden // 2 // hc
    half_T = T // 2
    dc = min(CHAIN_CHUNK, width)
    NP = width // dc
    bf16, f32 = jnp.bfloat16, jnp.float32
    dma = pltpu.SemaphoreType.DMA
    others = max(chips - 1, 1)
    scratch = [
        pltpu.VMEM((2, NJ, width, 2 * hc), bf16),
        pltpu.VMEM((2, 2, NJ, hc, width), bf16),
        pltpu.VMEM((T, width), bf16),
        pltpu.VMEM((T, width), f32),
        pltpu.VMEM((2, NJ, half_T, hc), f32),
        pltpu.VMEM((4, NJ, half_T, hc), bf16),
        pltpu.VMEM((4, NJ, half_T, hc), bf16),
        pltpu.VMEM((4, NJ, half_T, hc), bf16),
        pltpu.VMEM((4, others, NJ, half_T, hc), bf16),
        pltpu.VMEM((4, NJ, half_T, hc), bf16),
        pltpu.VMEM((4, NJ, half_T, hc), bf16),
        pltpu.VMEM((2, half_T, width), f32),
        pltpu.VMEM((4, NP, half_T, dc), bf16),
        pltpu.VMEM((4, NP, half_T, dc), bf16),
        pltpu.VMEM((4, NP, half_T, dc), bf16),
        pltpu.VMEM((4, 2, NP, half_T, dc), bf16),
        pltpu.VMEM((5, 8, T), f32),
        pltpu.VMEM((5, R - 1, 8, T), f32),
        pltpu.VMEM((T, LANES), f32),
        dma((2, 2, NJ)), dma((2, 2, NJ)),
        dma((4, NJ)), dma((4, NJ)),
        dma((4, others, NJ)), dma((4, others, NJ)),
        dma((4, NJ)), dma((4, NJ)),
        dma((4, NP)), dma((4, NP)),
        dma((4, 2, NP)), dma((4, 2, NP)),
        dma((5, R - 1)), dma((5, R - 1)),
    ]
    vmem, hbm = pl.BlockSpec(memory_space=pltpu.VMEM), pl.BlockSpec(memory_space=pl.ANY)
    return pl.pallas_call(
        functools.partial(kernel, R, C),
        out_shape=jax.ShapeDtypeStruct((T, width), bf16),
        in_specs=[vmem] * 4 + [hbm] * 4,
        out_specs=vmem,
        scratch_shapes=scratch,
        compiler_params=pltpu.CompilerParams(
            collective_id=0, has_side_effects=True, vmem_limit_bytes=60 * 1024 * 1024
        ),
    )(
        tokens, gain_1.reshape(1, width), gain_2.reshape(1, width), gain_3.reshape(1, width),
        up_1, down_1, up_2, down_2,
    )


def solution(mesh):
    in_specs = (
        P("grp", "ra"),
        P("ra"),
        P("ra", "cb"),
        P("cb", "ra"),
        P("ra"),
        P("ra", "cb"),
        P("cb", "ra"),
        P("ra"),
    )
    return jax.shard_map(
        functools.partial(per_device, mesh.shape["ra"], mesh.shape["cb"]),
        mesh=mesh, in_specs=in_specs, out_specs=P("grp", "ra"), check_vma=False,
    )
```
